32 devices in a mesh: ep: 8 (over z, x), tp: 4 (over y, core).
Axes of the slice: x: 2, y: 2, z: 4, core: 2. Of those that a mesh axis runs over, the one named last changes fastest.
Arguments:
- mixer_group_input: bfloat16 [2048, 1024], P('ep', 'tp'), may hold values from -6 to 6
- log_step_size: float32 [64, 2048], P('tp', 'ep'), may hold values from -16 to 0
- extra_log_decay: float32 [64, 2048], P('tp', 'ep'), may hold values from -0.7 to 0
- negated_eigen_real: float32 [64, 64], P('tp'), may hold values from 0.35 to 0.7
- frequency: float32 [64, 64], P('tp'), may hold values from 0 to 200
- group_input_matrices: bfloat16 [2, 64, 64, 16], P(None, 'tp'), may hold values from -1.5 to 1.5
- group_output_matrices: bfloat16 [2, 64, 16, 64], P(None, 'tp'), may hold values from -0.5 to 0.5
- channel_feedthrough: float32 [1024], P('tp'), may hold values from -3 to 3
- mixer_norm_scale: float32 [1024], replicated, may hold values from 0.1 to 1.9
- mixer_output_weight: bfloat16 [1024, 2048], P(None, 'tp'), may hold values from -0.1875 to 0.1875
- second_micro_input: bfloat16 [1024, 2048], P('ep'), may hold values from -6 to 6
- expert_norm_scale: float32 [2048], replicated, may hold values from 0.1 to 1.9
- routes: int32 [1024, 4], P('ep'), may hold values from 0 to 7, all different within a row; in each aligned block of 128 rows (0 to 127, 128 to 255, ...) at most 128 rows name the same one
- chosen_expert_weight: float32 [1024, 4], P('ep'), may hold values from 0.1 to 1
- expert_gate_weight: bfloat16 [8, 2048, 2048], P('ep', None, 'tp'), may hold values from -0.125 to 0.125
- expert_up_weight: bfloat16 [8, 2048, 2048], P('ep', None, 'tp'), may hold values from -0.125 to 0.125
- expert_down_weight: bfloat16 [8, 2048, 2048], P('ep', None, 'tp'), may hold values from -0.125 to 0.125
- shared_gate_weight: bfloat16 [2048, 2048], P(None, 'tp'), may hold values from -0.125 to 0.125
- shared_up_weight: bfloat16 [2048, 2048], P(None, 'tp'), may hold values from -0.125 to 0.125
- shared_down_weight: bfloat16 [2048, 2048], P(None, 'tp'), may hold values from -0.125 to 0.125
Outputs:
- mixed: bfloat16 [2048, 2048], P('ep', 'tp')
- moe_out: bfloat16 [1024, 2048], P('ep', 'tp')
The draws below stay inside these ranges and needn't reach their ends.
Inputs may be any that keep to these rules, and one draw needn't show every extreme that they name: `routes`: each row names 4 different experts; in each aligned block of 128 rows no expert is named by more than 128 rows, and in some block one expert is named by exactly 128 rows.
All inputs are finite; a program needn't handle non-finite values.
Results may differ from the reference program's by a relative error of at most 0.0068.
Values may be sent and summed in bfloat16 or wider, within the bound.
A program may use at most 192 MiB of HBM per device.

```python
import math
import jax
import jax.numpy as jnp
import numpy as np
from jax import lax

D = 2048
GROUPS = 64
GROUP_CH = 16
STATE = 64
WIDTH_SSM = 1024
FE = 2048
TOP_K = 4
TOKENS_PER_SHARD = 256
TOK_EP2 = 128
EXPERTS = 8
CAP = 128
TOKENS1 = 2048
TOKENS2 = 1024
N_EP = 8


def draw_log_step_size(key, part):
    base_key = jax.random.fold_in(key, 101)
    slow_key, fast_key, level_key, block_key, rough_key = jax.random.split(base_key, 5)
    slow_share = 0.5
    slow = jax.random.uniform(slow_key, (GROUPS,), jnp.float32) < slow_share
    fast_step = jax.random.uniform(fast_key, (GROUPS,), jnp.float32, 0.045, 0.09)
    slow_step = jax.random.uniform(level_key, (GROUPS,), jnp.float32, 0.15, 0.3) / (0.7 * TOKENS1)
    base = jnp.log(jnp.where(slow, slow_step, fast_step))
    block_count = TOKENS1 // TOKENS_PER_SHARD
    block_factor = jax.random.uniform(block_key, (GROUPS, block_count), jnp.float32, -0.7, 0.7)
    rough = jax.random.uniform(rough_key, (GROUPS, TOKENS1), jnp.float32, -0.4, 0.4)
    return base[:, None] + jnp.repeat(block_factor, TOKENS_PER_SHARD, axis=1) + rough


def draw_extra_log_decay(key, part):
    base_key = jax.random.fold_in(key, 202)
    place_key, size_key = jax.random.split(base_key)
    places = jax.random.randint(place_key, (GROUPS, 2), 0, TOKENS1)
    sizes_log = jnp.log(jax.random.uniform(size_key, (GROUPS, 2), jnp.float32, 0.5, 0.8))
    positions = jnp.arange(TOKENS1, dtype=jnp.int32)
    hits = positions[None, :, None] == places[:, None, :]
    return jnp.sum(jnp.where(hits, sizes_log[:, None, :], 0.0), axis=2)


def block_scale(key, extent, cuts, least, top_value):
    loudness = 1.0
    for dim, blocks in cuts:
        heights = jax.random.uniform(jax.random.fold_in(jax.random.fold_in(key, 6), dim), (blocks,), jnp.float32, least / len(cuts), top_value / len(cuts))
        loudness = loudness * jnp.repeat(jnp.exp(heights), extent[dim] // blocks).reshape((-1,) + (1,) * (len(extent) - 1 - dim))
    return loudness


def shared_out(rng, own, number, rows, count, top, limit, slope):
    ranking = jax.random.permutation(rng, count)
    heavy_load, usual = shares(count, rows * top, limit, slope, True), shares(count, rows * top, limit, slope, False)
    places = jnp.arange(count)

    def named(lengths, turn):
        used = int((lengths > 0).sum())
        fixed = max(1, used // 4)
        shifted = fixed + (places - fixed + turn * (used - fixed)) % max(1, count - fixed)
        return jnp.zeros((count,), jnp.int32).at[ranking[jnp.where(places < fixed, places, shifted)]].set(jnp.asarray(lengths, jnp.int32))

    lengths = jnp.where(number % 4 == 0, named(heavy_load, number // 4), named(usual, number - number // 4 - 1))
    mixed = jax.random.permutation(jax.random.fold_in(own, 3), count)
    donor, sink = mixed[0:count // 2 * 2:2], mixed[1:count // 2 * 2:2]
    room = jnp.minimum(lengths[donor] - 1, limit - lengths[sink]) // 2
    room = jnp.where((donor == ranking[0]) | (sink == ranking[0]) | (lengths[sink] == 0), 0, jnp.maximum(room, 0))
    shifted = jax.random.randint(jax.random.fold_in(own, 4), (count // 2,), 0, 1 << 20) % (room + 1)
    lengths = lengths.at[donor].add(-shifted).at[sink].add(shifted)
    members = jnp.searchsorted(jnp.cumsum(lengths), jnp.arange(rows * top), side="right").astype(jnp.int32)
    listing = members.reshape(top, rows).T
    listing = listing[jax.random.permutation(jax.random.fold_in(own, 1), rows)]
    turn = jax.random.randint(jax.random.fold_in(own, 2), (rows, 1), 0, top)
    return jnp.take_along_axis(listing, (jnp.arange(top)[None, :] + turn) % top, axis=1)


def shares(amount, total, reach, lean, full):
    weights = [(1 << 20) // math.isqrt(rank ** lean) + 1 for rank in range(1, amount + 1)]
    largest = reach if full else min(reach, max(-(-total // amount), total * weights[0] // sum(weights)))
    least = 1 if total - largest >= amount - 1 else 0
    counts, rest = [largest] + [least] * (amount - 1), total - largest - least * (amount - 1)
    while rest > 0:
        free = [i for i in range(1, amount) if counts[i] < largest] or [i for i in range(1, amount) if counts[i] < reach]
        mass, remaining = sum([weights[i] for i in free]), rest
        for i in free:
            more = min(reach - counts[i], max(1, remaining * weights[i] // mass), rest)
            counts[i] = counts[i] + more
            rest = rest - more
    return np.array(counts)


def normal_values(rng, extent, scale, most, cuts=(), held_as=jnp.bfloat16):
    drawn = jax.random.normal(rng, extent, jnp.float32) * scale
    if len(cuts) > 0:
        drawn = block_scale(rng, extent, cuts, -0.22, 0.18) * drawn
    return jnp.clip(drawn, min=-most, max=most).astype(held_as)


def setup_inputs(seed: int = 0) -> dict:
    key_of = jax.random.split(jax.random.key(seed), 21)
    mixer_group_input = normal_values(key_of[0], (TOKENS1, WIDTH_SSM), 1.0, 6.0, ((0, 8), (1, 4)))
    log_step_size = draw_log_step_size(jax.random.fold_in(key_of[20], 71), 0)
    extra_log_decay = draw_extra_log_decay(jax.random.fold_in(key_of[20], 71), 0)
    negated_eigen_real = jnp.clip(jnp.exp(math.log(0.7) - 0.6931472 * jax.random.uniform(key_of[3], (GROUPS, STATE), jnp.float32) ** block_scale(key_of[3], (GROUPS, STATE), ((0, 4),), -0.2, 0.2)), 0.35, 0.7)
    frequency = jnp.clip(200.0 * jax.random.uniform(key_of[4], (GROUPS, STATE), jnp.float32) ** block_scale(key_of[4], (GROUPS, STATE), ((0, 4),), -0.2, 0.2), 0.0, 200.0)
    group_input_matrices = normal_values(key_of[5], (2, GROUPS, STATE, GROUP_CH), GROUP_CH ** -0.5, 1.5, ((1, 4),))
    group_output_matrices = normal_values(key_of[6], (2, GROUPS, GROUP_CH, STATE), (2 * STATE) ** -0.5, 0.5, ((1, 4),))
    channel_feedthrough = normal_values(key_of[7], (WIDTH_SSM,), 0.5, 3.0, ((0, 4),), jnp.float32)
    mixer_norm_scale = jnp.clip(1.0 + 0.18 * jax.random.normal(key_of[8], (WIDTH_SSM,), jnp.float32), 0.1, 1.9)
    mixer_output_weight = normal_values(key_of[9], (WIDTH_SSM, D), WIDTH_SSM ** -0.5, 0.1875, ((1, 4),))
    second_micro_input = normal_values(key_of[10], (TOKENS2, D), 1.0, 6.0, ((0, 8),))
    expert_norm_scale = jnp.clip(1.0 + 0.18 * jax.random.normal(key_of[11], (D,), jnp.float32), 0.1, 1.9)
    routes_keys = jax.random.split(jax.random.fold_in(key_of[12], 1), TOKENS2 // TOK_EP2)
    routes_turns = jax.random.permutation(jax.random.fold_in(key_of[12], 3), TOKENS2 // TOK_EP2)
    routes = jax.vmap(lambda own, number: shared_out(jax.random.fold_in(key_of[12], 2), own, number, TOK_EP2, EXPERTS, TOP_K, CAP, 1))(routes_keys, routes_turns).reshape((TOKENS2, TOP_K))
    chosen_expert_weight = jnp.clip(jnp.exp(math.log(1.0) - 2.3025851 * jax.random.uniform(key_of[13], (TOKENS2, TOP_K), jnp.float32) ** block_scale(key_of[13], (TOKENS2, TOP_K), ((0, 8),), -0.2, 0.2)), 0.1, 1.0)
    expert_gate_weight = normal_values(key_of[14], (EXPERTS, D, FE), D ** -0.5, 0.125, ((0, 8), (2, 4)))
    expert_up_weight = normal_values(key_of[15], (EXPERTS, D, FE), D ** -0.5, 0.125, ((0, 8), (2, 4)))
    expert_down_weight = normal_values(key_of[16], (EXPERTS, FE, D), FE ** -0.5, 0.125, ((0, 8), (2, 4)))
    shared_gate_weight = normal_values(key_of[17], (D, FE), D ** -0.5, 0.125, ((1, 4),))
    shared_up_weight = normal_values(key_of[18], (D, FE), D ** -0.5, 0.125, ((1, 4),))
    shared_down_weight = normal_values(key_of[19], (FE, D), FE ** -0.5, 0.125, ((1, 4),))
    return {"mixer_group_input": mixer_group_input, "log_step_size": log_step_size, "extra_log_decay": extra_log_decay, "negated_eigen_real": negated_eigen_real, "frequency": frequency, "group_input_matrices": group_input_matrices, "group_output_matrices": group_output_matrices, "channel_feedthrough": channel_feedthrough, "mixer_norm_scale": mixer_norm_scale, "mixer_output_weight": mixer_output_weight, "second_micro_input": second_micro_input, "expert_norm_scale": expert_norm_scale, "routes": routes, "chosen_expert_weight": chosen_expert_weight, "expert_gate_weight": expert_gate_weight, "expert_up_weight": expert_up_weight, "expert_down_weight": expert_down_weight, "shared_gate_weight": shared_gate_weight, "shared_up_weight": shared_up_weight, "shared_down_weight": shared_down_weight}


eps_norm = 1e-06

def combine_steps(earlier, latter):
    return (earlier[0] * latter[0] - earlier[1] * latter[1], earlier[0] * latter[1] + earlier[1] * latter[0], latter[0] * earlier[2] - latter[1] * earlier[3] + latter[2], latter[0] * earlier[3] + latter[1] * earlier[2] + latter[3])

def local_states(inputs, step_logs, losses, negated_eigen_real, frequency, group_input_matrices):
    positions = inputs.shape[0]
    group_list = negated_eigen_real.shape[0]
    channels = inputs.reshape(positions, group_list, -1).astype(jnp.float32)
    step_size = jnp.exp(step_logs).T
    decay_log = -negated_eigen_real[None, :, :] * step_size[:, :, None]
    magnitude = jnp.exp(decay_log + losses.T[:, :, None])
    rotation = frequency[None, :, :] * step_size[:, :, None]
    scaling = jnp.sqrt(-jnp.expm1(2.0 * decay_log))
    driven = jnp.einsum('tgc,rgpc->rtgp', channels, group_input_matrices.astype(jnp.float32), precision=lax.Precision.HIGHEST)
    return lax.associative_scan(combine_steps, (magnitude * jnp.cos(rotation), magnitude * jnp.sin(rotation), scaling * driven[0], scaling * driven[1]), axis=0)

def readout(state_real_part, state_imaginary, group_output_matrices, inputs, channel_feedthrough):
    positions = state_real_part.shape[0]
    mapped_result = jnp.einsum('fnx,njx->fnj', state_real_part, group_output_matrices[0].astype(jnp.float32), precision=lax.Precision.HIGHEST)
    mapped_result = mapped_result - jnp.einsum('fnx,njx->fnj', state_imaginary, group_output_matrices[1].astype(jnp.float32), precision=lax.Precision.HIGHEST)
    total = mapped_result.reshape(positions, -1) + channel_feedthrough * inputs.astype(jnp.float32)
    return jax.nn.gelu(total).astype(jnp.bfloat16)

def scaled_rows(values, gain):
    widened = values.astype(jnp.float32)
    factor = lax.rsqrt(lax.optimization_barrier(jnp.mean(widened * widened, axis=-1, keepdims=True)) + eps_norm)
    return (widened * factor * gain).astype(jnp.bfloat16)

def slot_table(block_routes, experts, capacity):
    flat_routes = block_routes.reshape(-1)
    onehot = (flat_routes[:, None] == jnp.arange(experts, dtype=jnp.int32)[None, :]).astype(jnp.int32)
    earlier_count = lax.optimization_barrier(jnp.sum((jnp.cumsum(onehot, axis=0) - onehot) * onehot, axis=1))
    return (flat_routes * capacity + earlier_count).astype(jnp.int32)

def fill_slots(token_rows, slot_index, slot_count, top_count):
    owner_row = jnp.zeros((slot_count,), jnp.int32).at[slot_index].set(jnp.arange(slot_index.shape[0], dtype=jnp.int32) // top_count)
    occupied = jnp.zeros((slot_count,), jnp.int32).at[slot_index].set(1)
    return jnp.where(occupied[:, None] > 0, token_rows[owner_row], jnp.zeros((), token_rows.dtype))

def expert_block(token_rows, gate_weight, up_weight, down_weight):
    gate_part = jnp.dot(token_rows, gate_weight, preferred_element_type=jnp.float32)
    up_part = jnp.dot(token_rows, up_weight, preferred_element_type=jnp.float32)
    hidden = (jax.nn.silu(gate_part) * up_part).astype(jnp.bfloat16)
    return jnp.dot(hidden, down_weight, preferred_element_type=jnp.float32)

def reference(mixer_group_input, log_step_size, extra_log_decay, negated_eigen_real, frequency, group_input_matrices, group_output_matrices, channel_feedthrough, mixer_norm_scale, mixer_output_weight, second_micro_input, expert_norm_scale, routes, chosen_expert_weight, expert_gate_weight, expert_up_weight, expert_down_weight, shared_gate_weight, shared_up_weight, shared_down_weight):
    channel_count = mixer_group_input.shape[1]
    group_list, states = negated_eigen_real.shape
    block_inputs = mixer_group_input.reshape(N_EP, TOKENS_PER_SHARD, channel_count)
    block_steps = log_step_size.reshape(group_list, N_EP, TOKENS_PER_SHARD).transpose(1, 0, 2)
    block_decay_terms = extra_log_decay.reshape(group_list, N_EP, TOKENS_PER_SHARD).transpose(1, 0, 2)

    def one_block(incoming, pieces):
        inputs, step_logs, losses = pieces
        reach_real, reach_imag, state_real_part, state_imaginary = local_states(inputs, step_logs, losses, negated_eigen_real, frequency, group_input_matrices)
        state_real_part = state_real_part + reach_real * incoming[0] - reach_imag * incoming[1]
        state_imaginary = state_imaginary + reach_real * incoming[1] + reach_imag * incoming[0]
        outputs = readout(state_real_part, state_imaginary, group_output_matrices, inputs, channel_feedthrough)
        return ((state_real_part[-1], state_imaginary[-1]), outputs)
    empty_state = jnp.zeros((group_list, states), jnp.float32)
    _, outputs = lax.scan(one_block, (empty_state, empty_state), (block_inputs, block_steps, block_decay_terms))
    ssm_out = outputs.reshape(N_EP * TOKENS_PER_SHARD, channel_count)
    normed_mix = scaled_rows(ssm_out, mixer_norm_scale)
    mixed = jnp.dot(normed_mix, mixer_output_weight, preferred_element_type=jnp.float32).astype(jnp.bfloat16)
    normed_tokens = scaled_rows(second_micro_input, expert_norm_scale)
    block_rows = normed_tokens.reshape(N_EP, TOK_EP2, D)
    slot_index = jax.vmap(lambda routes_block: slot_table(routes_block, EXPERTS, CAP))(routes.reshape(N_EP, TOK_EP2, TOP_K))
    sent = jax.vmap(lambda rows_block, slots_block: fill_slots(rows_block, slots_block, EXPERTS * CAP, TOP_K))(block_rows, slot_index)
    sent = sent.reshape(N_EP, EXPERTS, CAP, D)

    def one_expert(expert):
        arrived = lax.dynamic_index_in_dim(sent, expert, axis=1, keepdims=False).reshape(N_EP * CAP, D)
        result = expert_block(arrived, expert_gate_weight[expert], expert_up_weight[expert], expert_down_weight[expert])
        return result.astype(jnp.bfloat16).reshape(N_EP, CAP, D)
    results = lax.map(one_expert, jnp.arange(EXPERTS, dtype=jnp.int32))
    returned = results.transpose(1, 0, 2, 3).reshape(N_EP, EXPERTS * CAP, D)
    picked = jax.vmap(lambda back_block, slots_block: back_block[slots_block])(returned, slot_index)
    picked = picked.reshape(N_EP * TOK_EP2, TOP_K, D).astype(jnp.float32)
    shared = expert_block(normed_tokens, shared_gate_weight, shared_up_weight, shared_down_weight)
    moe_out = (shared + lax.optimization_barrier(jnp.sum(picked * chosen_expert_weight[:, :, None], axis=1))).astype(jnp.bfloat16)
    return (mixed, moe_out)
```

```python
import jax
import jax.numpy as jnp
from jax import lax
from jax.experimental import pallas as pl
from jax.experimental.pallas import tpu as pltpu
from jax.sharding import PartitionSpec as P

eps_norm = 1e-06
LANES = 128
ROWS = 8


def cos_sin(angle):
    turns = jnp.floor(angle * 0.6366197723675814 + 0.5)
    rest = ((angle - turns * 1.5703125) - turns * 4.837512969970703125e-4) - turns * 7.549789954891882e-8
    square = rest * rest
    sine = rest + rest * square * (
        -1.6666654611e-1 + square * (8.3321608736e-3 + square * -1.9515295891e-4)
    )
    cosine = (
        1.0
        - 0.5 * square
        + square
        * square
        * (
            4.166664568298827e-2
            + square * (-1.388731625493765e-3 + square * 2.443315711809948e-5)
        )
    )
    quarter = turns.astype(jnp.int32)
    odd = (quarter & 1) == 1
    out_cos = jnp.where(odd, sine, cosine)
    out_sin = jnp.where(odd, cosine, sine)
    out_cos = jnp.where(((quarter + 1) & 2) == 2, -out_cos, out_cos)
    out_sin = jnp.where((quarter & 2) == 2, -out_sin, out_sin)
    return out_cos, out_sin


def one_minus_exp_neg(y):
    series = y * (
        1.0
        - y / 2
        * (1.0 - y / 3 * (1.0 - y / 4 * (1.0 - y / 5 * (1.0 - y / 6))))
    )
    return jnp.where(y < 0.3, series, 1.0 - jnp.exp(-y))


def scan_kernel(
    u_ref, win_ref, step_ref, loss_ref, eig_ref, freq_ref,
    reach_r_ref, reach_i_ref, state_r_ref, state_i_ref, ends_ref,
    ar_ref, ai_ref, br_ref, bi_ref,
):
    rows = u_ref.shape[0]
    u = u_ref[...]
    lane = lax.broadcasted_iota(jnp.int32, (rows, LANES), 1)
    half = lane < (LANES // step_ref.shape[2])
    step = jnp.where(half, step_ref[0, :, 0:1], step_ref[0, :, 1:2])
    loss = jnp.where(half, loss_ref[0, :, 0:1], loss_ref[0, :, 1:2])
    loss_rate = eig_ref[0] * step
    magnitude = jnp.exp(loss - loss_rate)
    cosine, sine = cos_sin(freq_ref[0] * step)
    scaling = jnp.sqrt(one_minus_exp_neg(2.0 * loss_rate))
    ar_ref[...] = magnitude * cosine
    ai_ref[...] = magnitude * sine
    br_ref[...] = scaling * jnp.dot(u, win_ref[0], preferred_element_type=jnp.float32)
    bi_ref[...] = scaling * jnp.dot(u, win_ref[1], preferred_element_type=jnp.float32)
    count = rows // ROWS
    reach = jnp.ones((ROWS, LANES), jnp.float32), jnp.zeros((ROWS, LANES), jnp.float32)
    state = jnp.zeros((ROWS, LANES), jnp.float32), jnp.zeros((ROWS, LANES), jnp.float32)
    for j in range(count):
        at = pl.ds(j * ROWS, ROWS)
        ar, ai, br, bi = ar_ref[at, :], ai_ref[at, :], br_ref[at, :], bi_ref[at, :]
        reach = ar * reach[0] - ai * reach[1], ar * reach[1] + ai * reach[0]
        state = ar * state[0] - ai * state[1] + br, ar * state[1] + ai * state[0] + bi
        ar_ref[at, :] = reach[0]
        ai_ref[at, :] = reach[1]
        br_ref[at, :] = state[0]
        bi_ref[at, :] = state[1]
    row = lax.broadcasted_iota(jnp.int32, (ROWS, LANES), 0)
    er, ei = jnp.ones((1, LANES), jnp.float32), jnp.zeros((1, LANES), jnp.float32)
    sr, si = jnp.zeros((1, LANES), jnp.float32), jnp.zeros((1, LANES), jnp.float32)
    pre_r, pre_i = reach[0] * 0.0, reach[0] * 0.0
    pre_sr, pre_si = pre_r, pre_r
    for s in range(ROWS):
        here = row == s
        pre_r = jnp.where(here, er, pre_r)
        pre_i = jnp.where(here, ei, pre_i)
        pre_sr = jnp.where(here, sr, pre_sr)
        pre_si = jnp.where(here, si, pre_si)
        tr, ti = reach[0][s : s + 1], reach[1][s : s + 1]
        ur, ui = state[0][s : s + 1], state[1][s : s + 1]
        er, ei, sr, si = (
            tr * er - ti * ei,
            tr * ei + ti * er,
            tr * sr - ti * si + ur,
            tr * si + ti * sr + ui,
        )
    for j in range(count):
        at = pl.ds(j * ROWS, ROWS)
        ar, ai = ar_ref[at, :], ai_ref[at, :]
        state_r_ref[at, :] = br_ref[at, :] + ar * pre_sr - ai * pre_si
        state_i_ref[at, :] = bi_ref[at, :] + ar * pre_si + ai * pre_sr
        reach_r_ref[at, :] = ar * pre_r - ai * pre_i
        reach_i_ref[at, :] = ar * pre_i + ai * pre_r
    ends_ref[0, 0:1] = er
    ends_ref[0, 1:2] = ei
    ends_ref[0, 2:3] = sr
    ends_ref[0, 3:4] = si


def read_kernel(
    hops, ends_ref, reach_r_ref, reach_i_ref, state_r_ref, state_i_ref, wout_ref, u_ref, feed_ref,
    out_ref, total_ref,
):
    tile = pl.program_id(0)
    place = jnp.full((1, LANES), lax.axis_index("ep"), jnp.int32)
    sr, si = jnp.zeros((1, LANES), jnp.float32), jnp.zeros((1, LANES), jnp.float32)
    for hop in range(hops - 1):
        keep = place > hop
        tr, ti = ends_ref[hop, 0, 0:1], ends_ref[hop, 0, 1:2]
        ur, ui = ends_ref[hop, 0, 2:3], ends_ref[hop, 0, 3:4]
        sr, si = (
            jnp.where(keep, tr * sr - ti * si + ur, sr),
            jnp.where(keep, tr * si + ti * sr + ui, si),
        )
    reach_r, reach_i = reach_r_ref[...], reach_i_ref[...]
    state_r = state_r_ref[...] + reach_r * sr - reach_i * si
    state_i = state_i_ref[...] + reach_r * si + reach_i * sr

    def product(state, weight):
        high = state.astype(jnp.bfloat16)
        low = (state - high.astype(jnp.float32)).astype(jnp.bfloat16)
        return jnp.dot(high, weight, preferred_element_type=jnp.float32) + jnp.dot(
            low, weight, preferred_element_type=jnp.float32
        )

    part = product(state_r, wout_ref[0]) - product(state_i, wout_ref[1])

    @pl.when(tile == 0)
    def _():
        total_ref[...] = part + feed_ref[...] * u_ref[...].astype(jnp.float32)

    @pl.when(tile > 0)
    def _():
        total_ref[...] += part

    @pl.when(tile == pl.num_programs(0) - 1)
    def _():
        value = total_ref[...]
        inner = 0.7978845608028654 * (value + 0.044715 * (value * value * value))
        out_ref[...] = (0.5 * value * (1.0 + jnp.tanh(inner))).astype(out_ref.dtype)


def mixer_local(
    inputs, step_logs, losses, eigen, frequency, group_in, group_out, feedthrough
):
    positions, channels = inputs.shape
    groups, states = eigen.shape
    width = groups * states
    tiles = width // LANES
    per_tile = groups // tiles
    seg = positions // ROWS

    def shuffled(rows):
        return rows.reshape(ROWS, seg, -1).transpose(1, 0, 2).reshape(positions, -1)

    def by_tile(table):
        wide = shuffled(table.T).reshape(positions, tiles, per_tile)
        return wide.transpose(1, 0, 2)

    u = shuffled(inputs)
    same = jnp.eye(groups, dtype=bool)
    zero = jnp.zeros((), group_in.dtype)
    win = jnp.where(
        same[None, :, None, :, None], group_in.transpose(0, 1, 3, 2)[:, :, :, None, :], zero
    ).reshape(2, channels, width)
    wout = jnp.where(
        same[None, :, None, :, None], group_out.transpose(0, 1, 3, 2)[:, :, :, None, :], zero
    ).reshape(2, width, channels)
    column = pl.BlockSpec((positions, LANES), lambda i: (0, i))
    whole_u = pl.BlockSpec((positions, channels), lambda i: (0, 0))
    pair = pl.BlockSpec((1, positions, per_tile), lambda i: (i, 0, 0))
    lane_row = pl.BlockSpec((1, 1, LANES), lambda i: (i, 0, 0))
    wide_shape = jax.ShapeDtypeStruct((positions, width), jnp.float32)
    column_scratch = pltpu.VMEM((positions, LANES), jnp.float32)
    reach_r, reach_i, state_r, state_i, ends = pl.pallas_call(
        scan_kernel,
        grid=(tiles,),
        in_specs=[
            whole_u,
            pl.BlockSpec((2, channels, LANES), lambda i: (0, 0, i)),
            pair,
            pair,
            lane_row,
            lane_row,
        ],
        out_specs=[column, column, column, column, pl.BlockSpec((1, 4, LANES), lambda i: (i, 0, 0))],
        out_shape=[wide_shape] * 4 + [jax.ShapeDtypeStruct((tiles, 4, LANES), jnp.float32)],
        scratch_shapes=[column_scratch] * 4,
        cost_estimate=pl.CostEstimate(
            flops=positions * channels * width * 4, bytes_accessed=24 * positions * width,
            transcendentals=4 * positions * width,
        ),
        name="scan_states",
    )(
        u,
        win,
        by_tile(jnp.exp(step_logs)),
        by_tile(losses),
        eigen.reshape(tiles, 1, LANES),
        frequency.reshape(tiles, 1, LANES),
    )
    hops = lax.axis_size("ep")
    all_ends = lax.all_gather(ends, "ep")
    out = pl.pallas_call(
        lambda *refs: read_kernel(hops, *refs),
        grid=(tiles,),
        in_specs=[
            pl.BlockSpec((hops, 1, 4, LANES), lambda i: (0, i, 0, 0)),
            column, column, column, column,
            pl.BlockSpec((2, LANES, channels), lambda i: (0, i, 0)),
            whole_u,
            pl.BlockSpec((1, channels), lambda i: (0, 0)),
        ],
        out_specs=whole_u,
        out_shape=jax.ShapeDtypeStruct((positions, channels), jnp.bfloat16),
        scratch_shapes=[pltpu.VMEM((positions, channels), jnp.float32)],
        cost_estimate=pl.CostEstimate(
            flops=positions * channels * width * 8, bytes_accessed=24 * positions * width,
            transcendentals=positions * channels,
        ),
        name="read_states",
    )(all_ends, reach_r, reach_i, state_r, state_i, wout, u, feedthrough.reshape(1, channels))
    return out.reshape(seg, ROWS, channels).transpose(1, 0, 2).reshape(positions, channels)


def scaled_rows(values, gain):
    widened = values.astype(jnp.float32)
    factor = lax.rsqrt(jnp.mean(widened * widened, axis=-1, keepdims=True) + eps_norm)
    return (widened * factor * gain).astype(jnp.bfloat16)


def gated(rows, gate_weight, up_weight):
    gate_part = jnp.dot(rows, gate_weight, preferred_element_type=jnp.float32)
    up_part = jnp.dot(rows, up_weight, preferred_element_type=jnp.float32)
    return (jax.nn.silu(gate_part) * up_part).astype(jnp.bfloat16)


def on_device(
    mixer_group_input,
    log_step_size,
    extra_log_decay,
    negated_eigen_real,
    frequency,
    group_input_matrices,
    group_output_matrices,
    channel_feedthrough,
    mixer_norm_scale,
    mixer_output_weight,
    second_micro_input,
    expert_norm_scale,
    routes,
    chosen_expert_weight,
    expert_gate_weight,
    expert_up_weight,
    expert_down_weight,
    shared_gate_weight,
    shared_up_weight,
    shared_down_weight,
):
    token_count, top_count = routes.shape
    experts = lax.axis_size("ep")
    column_count = expert_down_weight.shape[2]
    gate_weight, up_weight, down_weight = (
        expert_gate_weight[0],
        expert_up_weight[0],
        expert_down_weight[0],
    )
    normed_tokens = scaled_rows(second_micro_input, expert_norm_scale)
    all_tokens = lax.all_gather(normed_tokens, "ep", axis=0, tiled=True)
    ssm_out = mixer_local(
        mixer_group_input,
        log_step_size,
        extra_log_decay,
        negated_eigen_real,
        frequency,
        group_input_matrices,
        group_output_matrices,
        channel_feedthrough,
    )
    shared_hidden = gated(normed_tokens, shared_gate_weight, shared_up_weight)
    whole_rows = lax.all_gather(ssm_out, "tp", axis=1, tiled=True)
    whole_shared = lax.all_gather(shared_hidden, "tp", axis=1, tiled=True)
    hidden = gated(all_tokens, gate_weight, up_weight)
    whole_hidden = lax.all_gather(hidden, "tp", axis=1, tiled=True)
    normed_mix = scaled_rows(whole_rows, mixer_norm_scale)
    mixed = jnp.dot(normed_mix, mixer_output_weight, preferred_element_type=jnp.float32).astype(
        jnp.bfloat16
    )
    shared_columns = jnp.dot(
        whole_shared, shared_down_weight, preferred_element_type=jnp.float32
    )
    results = (
        jnp.dot(whole_hidden, down_weight, preferred_element_type=jnp.float32)
        .astype(jnp.bfloat16)
        .reshape(experts, token_count, column_count)
    )
    returned = lax.all_to_all(results, "ep", split_axis=0, concat_axis=0, tiled=True)
    share = jnp.sum(
        jnp.where(
            routes[:, :, None] == jnp.arange(experts, dtype=jnp.int32),
            chosen_expert_weight[:, :, None],
            0.0,
        ),
        axis=1,
    )
    combined = jnp.sum(returned.astype(jnp.float32) * share.T[:, :, None], axis=0)
    moe_out = (shared_columns + combined).astype(jnp.bfloat16)
    return (mixed, moe_out)


def solution(mesh):
    return jax.shard_map(
        on_device,
        mesh=mesh,
        in_specs=(
            P("ep", "tp"),
            P("tp", "ep"),
            P("tp", "ep"),
            P("tp", None),
            P("tp", None),
            P(None, "tp", None, None),
            P(None, "tp", None, None),
            P("tp"),
            P(),
            P(None, "tp"),
            P("ep", None),
            P(),
            P("ep", None),
            P("ep", None),
            P("ep", None, "tp"),
            P("ep", None, "tp"),
            P("ep", None, "tp"),
            P(None, "tp"),
            P(None, "tp"),
            P(None, "tp"),
        ),
        out_specs=(P("ep", "tp"), P("ep", "tp")),
        check_vma=False,
    )
```

```python
import jax
import jax.numpy as jnp
from jax import lax
from jax.experimental import pallas as pl
from jax.experimental.pallas import tpu as pltpu
from jax.sharding import PartitionSpec as P

eps_norm = 1e-06
LANES = 128
ROWS = 8


def cos_sin(angle):
    turns = jnp.floor(angle * 0.6366197723675814 + 0.5)
    rest = ((angle - turns * 1.5703125) - turns * 4.837512969970703125e-4) - turns * 7.549789954891882e-8
    square = rest * rest
    sine = rest + rest * square * (
        -1.6666654611e-1 + square * (8.3321608736e-3 + square * -1.9515295891e-4)
    )
    cosine = (
        1.0
        - 0.5 * square
        + square
        * square
        * (
            4.166664568298827e-2
            + square * (-1.388731625493765e-3 + square * 2.443315711809948e-5)
        )
    )
    quarter = turns.astype(jnp.int32)
    odd = (quarter & 1) == 1
    out_cos = jnp.where(odd, sine, cosine)
    out_sin = jnp.where(odd, cosine, sine)
    out_cos = jnp.where(((quarter + 1) & 2) == 2, -out_cos, out_cos)
    out_sin = jnp.where((quarter & 2) == 2, -out_sin, out_sin)
    return out_cos, out_sin


def one_minus_exp_neg(y):
    series = y * (
        1.0
        - y / 2
        * (1.0 - y / 3 * (1.0 - y / 4 * (1.0 - y / 5 * (1.0 - y / 6))))
    )
    return jnp.where(y < 0.3, series, 1.0 - jnp.exp(-y))


def scan_kernel(
    u_ref, win_ref, step_ref, loss_ref, eig_ref, freq_ref,
    reach_r_ref, reach_i_ref, state_r_ref, state_i_ref, ends_ref,
    ar_ref, ai_ref, br_ref, bi_ref,
):
    rows = u_ref.shape[0]
    u = u_ref[...]
    lane = lax.broadcasted_iota(jnp.int32, (rows, LANES), 1)
    half = lane < (LANES // step_ref.shape[2])
    step = jnp.where(half, step_ref[0, :, 0:1], step_ref[0, :, 1:2])
    loss = jnp.where(half, loss_ref[0, :, 0:1], loss_ref[0, :, 1:2])
    loss_rate = eig_ref[0] * step
    magnitude = jnp.exp(loss - loss_rate)
    cosine, sine = cos_sin(freq_ref[0] * step)
    scaling = jnp.sqrt(one_minus_exp_neg(2.0 * loss_rate))
    ar_ref[...] = magnitude * cosine
    ai_ref[...] = magnitude * sine
    br_ref[...] = scaling * jnp.dot(u, win_ref[0], preferred_element_type=jnp.float32)
    bi_ref[...] = scaling * jnp.dot(u, win_ref[1], preferred_element_type=jnp.float32)
    count = rows // ROWS
    reach = jnp.ones((ROWS, LANES), jnp.float32), jnp.zeros((ROWS, LANES), jnp.float32)
    state = jnp.zeros((ROWS, LANES), jnp.float32), jnp.zeros((ROWS, LANES), jnp.float32)
    for j in range(count):
        at = pl.ds(j * ROWS, ROWS)
        ar, ai, br, bi = ar_ref[at, :], ai_ref[at, :], br_ref[at, :], bi_ref[at, :]
        reach = ar * reach[0] - ai * reach[1], ar * reach[1] + ai * reach[0]
        state = ar * state[0] - ai * state[1] + br, ar * state[1] + ai * state[0] + bi
        ar_ref[at, :] = reach[0]
        ai_ref[at, :] = reach[1]
        br_ref[at, :] = state[0]
        bi_ref[at, :] = state[1]
    row = lax.broadcasted_iota(jnp.int32, (ROWS, LANES), 0)
    er, ei = jnp.ones((1, LANES), jnp.float32), jnp.zeros((1, LANES), jnp.float32)
    sr, si = jnp.zeros((1, LANES), jnp.float32), jnp.zeros((1, LANES), jnp.float32)
    pre_r, pre_i = reach[0] * 0.0, reach[0] * 0.0
    pre_sr, pre_si = pre_r, pre_r
    for s in range(ROWS):
        here = row == s
        pre_r = jnp.where(here, er, pre_r)
        pre_i = jnp.where(here, ei, pre_i)
        pre_sr = jnp.where(here, sr, pre_sr)
        pre_si = jnp.where(here, si, pre_si)
        tr, ti = reach[0][s : s + 1], reach[1][s : s + 1]
        ur, ui = state[0][s : s + 1], state[1][s : s + 1]
        er, ei, sr, si = (
            tr * er - ti * ei,
            tr * ei + ti * er,
            tr * sr - ti * si + ur,
            tr * si + ti * sr + ui,
        )
    for j in range(count):
        at = pl.ds(j * ROWS, ROWS)
        ar, ai = ar_ref[at, :], ai_ref[at, :]
        state_r_ref[at, :] = br_ref[at, :] + ar * pre_sr - ai * pre_si
        state_i_ref[at, :] = bi_ref[at, :] + ar * pre_si + ai * pre_sr
        reach_r_ref[at, :] = ar * pre_r - ai * pre_i
        reach_i_ref[at, :] = ar * pre_i + ai * pre_r
    ends_ref[0, 0:1] = er
    ends_ref[0, 1:2] = ei
    ends_ref[0, 2:3] = sr
    ends_ref[0, 3:4] = si


def read_kernel(
    hops, ends_ref, reach_r_ref, reach_i_ref, state_r_ref, state_i_ref, wout_ref, u_ref, feed_ref,
    out_ref, total_ref,
):
    tile = pl.program_id(0)
    place = jnp.full((1, LANES), lax.axis_index("ep"), jnp.int32)
    sr, si = jnp.zeros((1, LANES), jnp.float32), jnp.zeros((1, LANES), jnp.float32)
    for hop in range(hops - 1):
        keep = place > hop
        tr, ti = ends_ref[hop, 0, 0:1], ends_ref[hop, 0, 1:2]
        ur, ui = ends_ref[hop, 0, 2:3], ends_ref[hop, 0, 3:4]
        sr, si = (
            jnp.where(keep, tr * sr - ti * si + ur, sr),
            jnp.where(keep, tr * si + ti * sr + ui, si),
        )
    reach_r, reach_i = reach_r_ref[...], reach_i_ref[...]
    state_r = state_r_ref[...] + reach_r * sr - reach_i * si
    state_i = state_i_ref[...] + reach_r * si + reach_i * sr

    def product(state, weight):
        high = state.astype(jnp.bfloat16)
        low = (state - high.astype(jnp.float32)).astype(jnp.bfloat16)
        return jnp.dot(high, weight, preferred_element_type=jnp.float32) + jnp.dot(
            low, weight, preferred_element_type=jnp.float32
        )

    part = product(state_r, wout_ref[0]) - product(state_i, wout_ref[1])

    @pl.when(tile == 0)
    def _():
        total_ref[...] = part + feed_ref[...] * u_ref[...].astype(jnp.float32)

    @pl.when(tile > 0)
    def _():
        total_ref[...] += part

    @pl.when(tile == pl.num_programs(0) - 1)
    def _():
        value = total_ref[...]
        inner = 0.7978845608028654 * (value + 0.044715 * (value * value * value))
        out_ref[...] = (0.5 * value * (1.0 + jnp.tanh(inner))).astype(out_ref.dtype)


def mixer_local(
    inputs, step_logs, losses, eigen, frequency, group_in, group_out, feedthrough
):
    positions, channels = inputs.shape
    groups, states = eigen.shape
    width = groups * states
    tiles = width // LANES
    per_tile = groups // tiles
    seg = positions // ROWS

    def shuffled(rows):
        return rows.reshape(ROWS, seg, -1).transpose(1, 0, 2).reshape(positions, -1)

    def by_tile(table):
        wide = shuffled(table.T).reshape(positions, tiles, per_tile)
        return wide.transpose(1, 0, 2)

    u = shuffled(inputs)
    same = jnp.eye(groups, dtype=bool)
    zero = jnp.zeros((), group_in.dtype)
    win = jnp.where(
        same[None, :, None, :, None], group_in.transpose(0, 1, 3, 2)[:, :, :, None, :], zero
    ).reshape(2, channels, width)
    wout = jnp.where(
        same[None, :, None, :, None], group_out.transpose(0, 1, 3, 2)[:, :, :, None, :], zero
    ).reshape(2, width, channels)
    column = pl.BlockSpec((positions, LANES), lambda i: (0, i))
    whole_u = pl.BlockSpec((positions, channels), lambda i: (0, 0))
    pair = pl.BlockSpec((1, positions, per_tile), lambda i: (i, 0, 0))
    lane_row = pl.BlockSpec((1, 1, LANES), lambda i: (i, 0, 0))
    wide_shape = jax.ShapeDtypeStruct((positions, width), jnp.float32)
    column_scratch = pltpu.VMEM((positions, LANES), jnp.float32)
    reach_r, reach_i, state_r, state_i, ends = pl.pallas_call(
        scan_kernel,
        grid=(tiles,),
        in_specs=[
            whole_u,
            pl.BlockSpec((2, channels, LANES), lambda i: (0, 0, i)),
            pair,
            pair,
            lane_row,
            lane_row,
        ],
        out_specs=[column, column, column, column, pl.BlockSpec((1, 4, LANES), lambda i: (i, 0, 0))],
        out_shape=[wide_shape] * 4 + [jax.ShapeDtypeStruct((tiles, 4, LANES), jnp.float32)],
        scratch_shapes=[column_scratch] * 4,
        cost_estimate=pl.CostEstimate(
            flops=positions * channels * width * 4, bytes_accessed=24 * positions * width,
            transcendentals=4 * positions * width,
        ),
        name="scan_states",
    )(
        u,
        win,
        by_tile(jnp.exp(step_logs)),
        by_tile(losses),
        eigen.reshape(tiles, 1, LANES),
        frequency.reshape(tiles, 1, LANES),
    )
    hops = lax.axis_size("ep")
    all_ends = lax.all_gather(ends, "ep")
    out = pl.pallas_call(
        lambda *refs: read_kernel(hops, *refs),
        grid=(tiles,),
        in_specs=[
            pl.BlockSpec((hops, 1, 4, LANES), lambda i: (0, i, 0, 0)),
            column, column, column, column,
            pl.BlockSpec((2, LANES, channels), lambda i: (0, i, 0)),
            whole_u,
            pl.BlockSpec((1, channels), lambda i: (0, 0)),
        ],
        out_specs=whole_u,
        out_shape=jax.ShapeDtypeStruct((positions, channels), jnp.bfloat16),
        scratch_shapes=[pltpu.VMEM((positions, channels), jnp.float32)],
        cost_estimate=pl.CostEstimate(
            flops=positions * channels * width * 8, bytes_accessed=24 * positions * width,
            transcendentals=positions * channels,
        ),
        name="read_states",
    )(all_ends, reach_r, reach_i, state_r, state_i, wout, u, feedthrough.reshape(1, channels))
    return out.reshape(seg, ROWS, channels).transpose(1, 0, 2).reshape(positions, channels)


def scaled_rows(values, gain):
    widened = values.astype(jnp.float32)
    factor = lax.rsqrt(jnp.mean(widened * widened, axis=-1, keepdims=True) + eps_norm)
    return (widened * factor * gain).astype(jnp.bfloat16)


def gated(rows, gate_weight, up_weight):
    gate_part = jnp.dot(rows, gate_weight, preferred_element_type=jnp.float32)
    up_part = jnp.dot(rows, up_weight, preferred_element_type=jnp.float32)
    return (jax.nn.silu(gate_part) * up_part).astype(jnp.bfloat16)


def on_device(
    mixer_group_input,
    log_step_size,
    extra_log_decay,
    negated_eigen_real,
    frequency,
    group_input_matrices,
    group_output_matrices,
    channel_feedthrough,
    mixer_norm_scale,
    mixer_output_weight,
    second_micro_input,
    expert_norm_scale,
    routes,
    chosen_expert_weight,
    expert_gate_weight,
    expert_up_weight,
    expert_down_weight,
    shared_gate_weight,
    shared_up_weight,
    shared_down_weight,
):
    token_count, top_count = routes.shape
    experts = lax.axis_size("ep")
    column_count = expert_down_weight.shape[2]
    gate_weight, up_weight, down_weight = (
        expert_gate_weight[0],
        expert_up_weight[0],
        expert_down_weight[0],
    )
    normed_tokens = scaled_rows(second_micro_input, expert_norm_scale)
    model_width = normed_tokens.shape[1]
    part = lax.rem(lax.axis_index("tp"), 2)
    own_half = lax.dynamic_slice_in_dim(
        normed_tokens, part * (model_width // 2), model_width // 2, 1
    )
    half_tokens = lax.all_gather(own_half, "ep", axis=0, tiled=True)
    pairs = [[2 * i, 2 * i + 1] for i in range(lax.axis_size("tp") // 2)]
    all_tokens = lax.all_gather(
        half_tokens, "tp", axis=1, tiled=True, axis_index_groups=pairs
    )
    ssm_out = mixer_local(
        mixer_group_input,
        log_step_size,
        extra_log_decay,
        negated_eigen_real,
        frequency,
        group_input_matrices,
        group_output_matrices,
        channel_feedthrough,
    )
    shared_hidden = gated(normed_tokens, shared_gate_weight, shared_up_weight)
    whole_rows = lax.all_gather(ssm_out, "tp", axis=1, tiled=True)
    whole_shared = lax.all_gather(shared_hidden, "tp", axis=1, tiled=True)
    hidden = gated(all_tokens, gate_weight, up_weight)
    whole_hidden = lax.all_gather(hidden, "tp", axis=1, tiled=True)
    normed_mix = scaled_rows(whole_rows, mixer_norm_scale)
    mixed = jnp.dot(normed_mix, mixer_output_weight, preferred_element_type=jnp.float32).astype(
        jnp.bfloat16
    )
    shared_columns = jnp.dot(
        whole_shared, shared_down_weight, preferred_element_type=jnp.float32
    )
    results = (
        jnp.dot(whole_hidden, down_weight, preferred_element_type=jnp.float32)
        .astype(jnp.bfloat16)
        .reshape(experts, token_count, column_count)
    )
    returned = lax.all_to_all(results, "ep", split_axis=0, concat_axis=0, tiled=True)
    share = jnp.sum(
        jnp.where(
            routes[:, :, None] == jnp.arange(experts, dtype=jnp.int32),
            chosen_expert_weight[:, :, None],
            0.0,
        ),
        axis=1,
    )
    combined = jnp.sum(returned.astype(jnp.float32) * share.T[:, :, None], axis=0)
    moe_out = (shared_columns + combined).astype(jnp.bfloat16)
    return (mixed, moe_out)


def solution(mesh):
    return jax.shard_map(
        on_device,
        mesh=mesh,
        in_specs=(
            P("ep", "tp"),
            P("tp", "ep"),
            P("tp", "ep"),
            P("tp", None),
            P("tp", None),
            P(None, "tp", None, None),
            P(None, "tp", None, None),
            P("tp"),
            P(),
            P(None, "tp"),
            P("ep", None),
            P(),
            P("ep", None),
            P("ep", None),
            P("ep", None, "tp"),
            P("ep", None, "tp"),
            P("ep", None, "tp"),
            P(None, "tp"),
            P(None, "tp"),
            P(None, "tp"),
        ),
        out_specs=(P("ep", "tp"), P("ep", "tp")),
        check_vma=False,
    )
```
